32 devices in a mesh: grp: 2 (over y), sp: 4 (over z), tp: 4 (over x, core).
Axes of the slice: x: 2, y: 2, z: 4, core: 2. Of those that a mesh axis runs over, the one named last changes fastest.
Arguments:
- resid_in: bfloat16 [8, 256, 2048], P(('grp', 'tp'), 'sp'), parts along dimension 0, may hold values from -6 to 6
- query_one: bfloat16 [8, 256, 1024], P('grp', 'sp', 'tp'), parts along dimension 0, may hold values from -624 to 624
- key_one: bfloat16 [8, 256, 256], P('grp', 'sp', 'tp'), parts along dimension 0, may hold values from -7.78125 to 7.78125
- query_two: bfloat16 [8, 256, 1024], P('grp', 'sp', 'tp'), parts along dimension 0, may hold values from -624 to 624
- key_two: bfloat16 [8, 256, 256], P('grp', 'sp', 'tp'), parts along dimension 0, may hold values from -7.78125 to 7.78125
- value: bfloat16 [8, 256, 512], P('grp', 'sp', 'tp'), parts along dimension 0, may hold values from -6 to 6
- lam: float32 [32], P('tp'), may hold values from 0.3 to 0.8
- head_gain: float32 [64], replicated, may hold values from 0.1 to 1.9
- doc_ids: int32 [8, 256], P('grp', 'sp'), parts along dimension 0, may hold values from 0 to 3, never falling along the last dimension, each value on 1 to 128 neighbouring positions
- out_weight: bfloat16 [2048, 2048], P('tp'), may hold values from -0.125 to 0.125
- norm_gain: float32 [2048], replicated, may hold values from 0.1 to 1.9
- gate_weight: bfloat16 [2048, 5632], P('sp', 'tp'), may hold values from -0.125 to 0.125
- value_weight: bfloat16 [2048, 5632], P('sp', 'tp'), may hold values from -0.125 to 0.125
- conv_gate: float32 [3, 5632], P(None, 'tp'), may hold values from -3.5 to 3.5
- conv_value: float32 [3, 5632], P(None, 'tp'), may hold values from -3.5 to 3.5
- down_weight: bfloat16 [5632, 2048], P('tp', 'sp'), may hold values from -0.078125 to 0.078125
Outputs:
- resid_out: bfloat16 [8, 256, 2048], P(('grp', 'tp'), 'sp'), parts along dimension 0
The draws below stay inside these ranges and needn't reach their ends.
There are 2 independent parts, one for each index of `grp`. The reference program is written for one: setup_inputs(seed, part) draws one part's arguments, and reference() takes and returns one part's arrays. A program takes and returns all parts, laid end to end along the dimension named above; an argument that names none is the same for every part. Nothing has to cross between parts.
All inputs are finite; a program needn't handle non-finite values.
Results may differ from the reference program's by a relative error of at most 0.014.
Values may be sent and summed in bfloat16 or wider, within the bound.
A program may use at most 128 MiB of HBM per device.

```python
import math
import jax
import jax.numpy as jnp
import numpy as np
from jax import lax

D = 2048
HEADS = 32
KV_HEADS = 8
QK = 32
HEAD_DIM = 64
FF = 5632
SEQS = 4
SEQ_LEN = 256
N_TP = 4


def drawn_queries(key):
    base = 1.3 * jax.random.normal(jax.random.fold_in(key, 11), (SEQS, SEQ_LEN, HEADS * QK), jnp.float32)
    base = jnp.clip(base, -7.8, 7.8)
    return base.astype(jnp.bfloat16)


def draw_query_one(key, part):
    return drawn_queries(jax.random.fold_in(key, 1))


def draw_query_two(key, part):
    return drawn_queries(jax.random.fold_in(key, 2))


def block_levels(own_key, shape, cuts, least, largest):
    level = 1.0
    for axis_at, parts in cuts:
        steps = jax.random.uniform(jax.random.fold_in(jax.random.fold_in(own_key, 6), axis_at), (parts,), jnp.float32, least / len(cuts), largest / len(cuts))
        level = level * jnp.repeat(jnp.exp(steps), shape[axis_at] // parts).reshape((-1,) + (1,) * (len(shape) - 1 - axis_at))
    return level


def length_profile(number_of, total, most, lean):
    portions = [(1 << 20) // math.isqrt(rank ** lean) + 1 for rank in range(2, number_of + 1)]
    spare, holding = total - most - (number_of - 1), [1] * (number_of - 1)
    while spare > 0:
        movable = [i for i in range(number_of - 1) if holding[i] < most]
        pool, left = sum([portions[i] for i in movable]), spare
        for i in movable:
            addition = min(most - holding[i], max(1, left * portions[i] // pool), spare)
            holding[i] = holding[i] + addition
            spare = spare - addition
    return np.array([most] + holding)


def ragged(own_key, amount, total, limit, slope):
    if amount == 2:
        one = jax.random.randint(own_key, (), max(1, total - limit), min(limit, total - 1) + 1)
        return jnp.stack([one, total - one])
    lengths = jnp.asarray(length_profile(amount, total, limit, slope), jnp.int32)
    twos = (amount - 1) // 2
    giver, sink = lengths[1:1 + 2 * twos:2], lengths[2:2 + 2 * twos:2]
    margin = jnp.minimum(giver - 1, limit - sink)
    shifted = jax.random.randint(jax.random.fold_in(own_key, 1), (twos,), 0, 1 << 20) % (margin + 1)
    lengths = lengths.at[1:1 + 2 * twos:2].set(giver - shifted).at[2:2 + 2 * twos:2].set(sink + shifted)
    return lengths[jax.random.permutation(jax.random.fold_in(own_key, 2), amount)]


def noise(stream_key, extent, scale, bound, pieces=(), kind=jnp.bfloat16):
    drawn = scale * jax.random.normal(stream_key, extent, jnp.float32)
    if pieces:
        drawn = drawn * block_levels(stream_key, extent, pieces, -0.22, 0.18)
    return jnp.clip(drawn, -bound, bound).astype(kind)


def setup_inputs(seed: int = 0, part: int = 0) -> dict:
    arg_keys = jax.random.split(jax.random.key(seed), 17)
    part_keys = jax.random.split(jax.random.fold_in(arg_keys[16], part), 17)
    resid_in = noise(part_keys[0], (SEQS, SEQ_LEN, D), 1.0, 6.0, ((0, 4), (1, 4)))
    query_one = draw_query_one(jax.random.fold_in(jax.random.fold_in(arg_keys[16], part), 71), part)
    key_one = noise(part_keys[2], (SEQS, SEQ_LEN, KV_HEADS * QK), 1.3, 7.78125, ((1, 4), (2, 4)))
    query_two = draw_query_two(jax.random.fold_in(jax.random.fold_in(arg_keys[16], part), 71), part)
    key_two = noise(part_keys[4], (SEQS, SEQ_LEN, KV_HEADS * QK), 1.3, 7.78125, ((1, 4), (2, 4)))
    value = noise(part_keys[5], (SEQS, SEQ_LEN, KV_HEADS * HEAD_DIM), 1.0, 6.0, ((1, 4), (2, 4)))
    lam = jnp.clip(0.3 + 0.5 * jax.random.uniform(arg_keys[6], (HEADS,), jnp.float32) ** block_levels(arg_keys[6], (HEADS,), ((0, 4),), -0.2, 0.2), 0.3, 0.8)
    head_gain = jnp.clip(1.0 + 0.18 * jax.random.normal(arg_keys[7], (HEAD_DIM,), jnp.float32), 0.1, 1.9)
    doc_ids = jax.vmap(lambda own: jnp.searchsorted(jnp.cumsum(ragged(own, 4, SEQ_LEN, SEQ_LEN // 2, 1)), jnp.arange(SEQ_LEN), side="right"))(jax.random.split(part_keys[8], SEQS)).reshape((SEQS, SEQ_LEN)).astype(jnp.int32)
    out_weight = noise(arg_keys[9], (HEADS * HEAD_DIM, D), (HEADS * HEAD_DIM) ** -0.5, 0.125, ((0, 4),))
    norm_gain = jnp.clip(1.0 + 0.18 * jax.random.normal(arg_keys[10], (D,), jnp.float32), 0.1, 1.9)
    gate_weight = noise(arg_keys[11], (D, FF), D ** -0.5, 0.125, ((0, 4), (1, 4)))
    value_weight = noise(arg_keys[12], (D, FF), D ** -0.5, 0.125, ((0, 4), (1, 4)))
    conv_gate = noise(arg_keys[13], (3, FF), 3 ** -0.5, 3.5, ((1, 4),), jnp.float32)
    conv_value = noise(arg_keys[14], (3, FF), 3 ** -0.5, 3.5, ((1, 4),), jnp.float32)
    down_weight = noise(arg_keys[15], (FF, D), FF ** -0.5, 0.078125, ((0, 4), (1, 4)))
    return dict(resid_in=resid_in, query_one=query_one, key_one=key_one, query_two=query_two, key_two=key_two, value=value, lam=lam, head_gain=head_gain, doc_ids=doc_ids, out_weight=out_weight, norm_gain=norm_gain, gate_weight=gate_weight, value_weight=value_weight, conv_gate=conv_gate, conv_value=conv_value, down_weight=down_weight)


NEG_BIG = -1e+30
NORM_EPS = 1e-06
ROPE_BASE = 500000.0

def rotate(block, positions, heads):
    entries = block.astype(jnp.float32).reshape(block.shape[:-1] + (heads, -1))
    width = entries.shape[-1]
    half = width // 2
    freqs = ROPE_BASE ** (-jnp.arange(half, dtype=jnp.float32) * 2.0 / width)
    angles = positions.astype(jnp.float32)[:, None] * freqs[None, :]
    cosine = jnp.cos(angles)[:, None, :]
    sine = jnp.sin(angles)[:, None, :]
    first = entries[..., :half]
    second = entries[..., half:]
    turned = jnp.concatenate([first * cosine - second * sine, second * cosine + first * sine], axis=-1)
    return turned.astype(jnp.bfloat16)

def depthwise(edge, current, taps, edge_docs, docs):
    count = current.shape[0]
    extended = jnp.concatenate([edge, current], axis=0).astype(jnp.float32)
    ext_docs = jnp.concatenate([edge_docs, docs], axis=0)
    total = taps[2][None, :] * extended[2:]
    for shift_k in range(2):
        same = (ext_docs[shift_k:shift_k + count] == docs)[:, None]
        total = total + jnp.where(same, taps[shift_k][None, :] * extended[shift_k:shift_k + count], 0.0)
    return total

def head_rows(args, positions, docs, gain):
    q_one, k_one, q_two, k_two, vals, weight = args
    tokens = vals.shape[0]
    blk = math.gcd(tokens, 512)
    scale = q_one.shape[-1] ** (-0.5)

    def one_block(index):
        start = index * blk
        qpos = start + jnp.arange(blk, dtype=jnp.int32)
        qdoc = lax.dynamic_slice_in_dim(docs, start, blk, 0)
        allowed = (positions[None, :] <= qpos[:, None]) & (docs[None, :] == qdoc[:, None])

        def branch(q_all, k_all):
            qblock = lax.dynamic_slice_in_dim(q_all, start, blk, 0)
            scores = jnp.dot(qblock, k_all.T, preferred_element_type=jnp.float32) * scale
            scores = jnp.where(allowed, scores, NEG_BIG)
            peak = lax.optimization_barrier(jnp.max(scores, axis=-1, keepdims=True))
            expd = jnp.where(allowed, jnp.exp(scores - peak), 0.0)
            numer = jnp.dot(expd.astype(jnp.bfloat16), vals, preferred_element_type=jnp.float32)
            return numer / lax.optimization_barrier(jnp.sum(expd, axis=-1, keepdims=True))
        mixed = branch(q_one, k_one) - weight * branch(q_two, k_two)
        meansq = lax.optimization_barrier(jnp.mean(mixed * mixed, axis=-1, keepdims=True))
        return (mixed * lax.rsqrt(meansq + NORM_EPS) * gain[None, :]).astype(jnp.bfloat16)
    out = lax.map(one_block, jnp.arange(tokens // blk))
    return out.reshape(tokens, -1)

def grouped_product(left, right, groups):
    width = left.shape[1] // groups
    total = jnp.zeros((left.shape[0], right.shape[1]), jnp.float32)
    for group in range(groups):
        part = jnp.dot(left[:, group * width:(group + 1) * width], right[group * width:(group + 1) * width], preferred_element_type=jnp.float32).astype(jnp.bfloat16)
        part = lax.optimization_barrier(part)
        total = total + part.astype(jnp.float32)
    return total

def reference(resid_in, query_one, key_one, query_two, key_two, value, lam, head_gain, doc_ids, out_weight, norm_gain, gate_weight, value_weight, conv_gate, conv_value, down_weight):
    heads = lam.shape[0]
    key_width = query_one.shape[2] // heads
    kv_heads = key_one.shape[2] // key_width
    group = heads // kv_heads

    def by_head(block):
        return jnp.transpose(block, (1, 0, 2))

    def one_sequence(args):
        resid, q_a, k_a, q_b, k_b, vals_in, docs = args
        tokens = resid.shape[0]
        positions = jnp.arange(tokens, dtype=jnp.int32)
        q_first = by_head(rotate(q_a, positions, heads))
        k_first = jnp.repeat(by_head(rotate(k_a, positions, kv_heads)), group, axis=0)
        q_second = by_head(rotate(q_b, positions, heads))
        k_second = jnp.repeat(by_head(rotate(k_b, positions, kv_heads)), group, axis=0)
        vals = jnp.repeat(by_head(vals_in.reshape(tokens, kv_heads, -1)), group, axis=0)
        per_head = lax.map(lambda items: head_rows(items, positions, docs, head_gain), (q_first, k_first, q_second, k_second, vals, lam))
        heads_out = jnp.transpose(per_head, (1, 0, 2)).reshape(tokens, -1)
        proj = grouped_product(heads_out, out_weight, N_TP)
        mid = resid.astype(jnp.float32) + proj
        meansq = lax.optimization_barrier(jnp.mean(mid * mid, axis=-1, keepdims=True))
        normed = (mid * lax.rsqrt(meansq + NORM_EPS) * norm_gain[None, :]).astype(jnp.bfloat16)
        up_gate = jnp.dot(normed, gate_weight, preferred_element_type=jnp.float32).astype(jnp.bfloat16)
        up_value = jnp.dot(normed, value_weight, preferred_element_type=jnp.float32).astype(jnp.bfloat16)
        edge = jnp.zeros((2, up_gate.shape[1]), jnp.bfloat16)
        edge_docs = jnp.full((2,), -1, jnp.int32)
        conv_g = depthwise(edge, up_gate, conv_gate, edge_docs, docs)
        conv_v = depthwise(edge, up_value, conv_value, edge_docs, docs)
        hidden = (jax.nn.silu(conv_g) * conv_v).astype(jnp.bfloat16)
        down = grouped_product(hidden, down_weight, N_TP)
        return (mid + down).astype(jnp.bfloat16)
    return lax.map(one_sequence, (resid_in, query_one, key_one, query_two, key_two, value, doc_ids))
```

```python
import math

import jax
import jax.numpy as jnp
from jax import lax
from jax.sharding import PartitionSpec as P

NEG_BIG = -1e30
NORM_EPS = 1e-06
ROPE_BASE = 500000.0


def rotate(block, positions, heads):
    entries = block.astype(jnp.float32).reshape(block.shape[:-1] + (heads, -1))
    width = entries.shape[-1]
    half = width // 2
    freqs = ROPE_BASE ** (-jnp.arange(half, dtype=jnp.float32) * 2.0 / width)
    angles = positions.astype(jnp.float32)[:, None] * freqs[None, :]
    cosine = jnp.cos(angles)[:, None, :]
    sine = jnp.sin(angles)[:, None, :]
    first = entries[..., :half]
    second = entries[..., half:]
    turned = jnp.concatenate(
        [first * cosine - second * sine, second * cosine + first * sine], axis=-1
    )
    return turned.astype(jnp.bfloat16)


def depthwise(current, taps, docs):
    shown = current.astype(jnp.float32)
    total = taps[2] * shown
    for back in (1, 2):
        moved = jnp.pad(shown, ((0, 0), (back, 0), (0, 0)))[:, : shown.shape[1]]
        moved_docs = jnp.pad(docs, ((0, 0), (back, 0)), constant_values=-1)[:, : docs.shape[1]]
        total = total + jnp.where((moved_docs == docs)[..., None], taps[2 - back] * moved, 0.0)
    return total


def cyclic(array, axis, by):
    length = lax.axis_size(axis)
    return lax.ppermute(array, axis, [(i, (i + by) % length) for i in range(length)])


def exchange(pieces):
    count = lax.axis_size("sp")
    copies = lax.axis_size("grp")
    me = lax.axis_index("sp")
    mine = lax.axis_index("grp")
    if count > 8:
        return lax.all_to_all(pieces, "sp", 0, 0)
    shared = pieces.reshape(count, copies, pieces.shape[1] // copies, *pieces.shape[2:])
    by_shift = [lax.dynamic_index_in_dim(pieces, me, 0, keepdims=False)]
    for shift in range(1, count):
        dest = lax.rem(me + shift, count)
        part = lax.dynamic_slice(
            shared, (dest, mine) + (0,) * (shared.ndim - 2), (1, 1) + shared.shape[2:]
        )[0, 0]
        got = [cyclic(part, "sp", shift)]
        for turn in range(1, copies):
            got.append(cyclic(got[0], "grp", turn))
        got = jnp.stack(got, axis=0)
        order = [lax.rem(mine - share + copies, copies) for share in range(copies)]
        got = jnp.stack([lax.dynamic_index_in_dim(got, at, 0, keepdims=False) for at in order])
        by_shift.append(got.reshape(pieces.shape[1:]))
    stacked = jnp.stack(by_shift, axis=0)
    return jnp.stack(
        [
            lax.dynamic_index_in_dim(stacked, lax.rem(me - source + count, count), 0, keepdims=False)
            for source in range(count)
        ],
        axis=0,
    )


def online_step(state, queries, keys, vals, allowed, scale):
    peak, total, accum = state
    scores = (
        jnp.einsum("sqhgd,skhd->shgqk", queries, keys, preferred_element_type=jnp.float32) * scale
    )
    mask = allowed[:, None, None]
    scores = jnp.where(mask, scores, NEG_BIG)
    new_peak = jnp.maximum(peak, jnp.max(scores, axis=-1))
    expd = jnp.where(mask, jnp.exp(scores - new_peak[..., None]), 0.0)
    fade = jnp.exp(peak - new_peak)
    new_total = total * fade + jnp.sum(expd, axis=-1)
    update = jnp.einsum(
        "shgqk,skhd->shgqd", expd.astype(jnp.bfloat16), vals, preferred_element_type=jnp.float32
    )
    return (new_peak, new_total, accum * fade[..., None] + update)


def per_device(
    resid_in,
    query_one,
    key_one,
    query_two,
    key_two,
    value,
    lam,
    head_gain,
    doc_ids,
    out_weight,
    norm_gain,
    gate_weight,
    value_weight,
    conv_gate,
    conv_value,
    down_weight,
):
    n_sp = lax.axis_size("sp")
    me = lax.axis_index("sp")
    depth, width = gate_weight.shape
    share = width // n_sp
    up_pieces = jnp.stack([gate_weight, value_weight], axis=1).reshape(depth, 2, n_sp, share)
    up_all = exchange(jnp.transpose(up_pieces, (2, 0, 1, 3)))
    down_all = exchange(down_weight.reshape(n_sp, share, down_weight.shape[1]))
    up_all = up_all.reshape(n_sp * depth, 2, share)
    down_full = jnp.transpose(down_all, (1, 0, 2)).reshape(share, -1)
    seqs = query_one.shape[0]
    rows = query_one.shape[1]
    heads = lam.shape[0]
    key_width = query_one.shape[2] // heads
    kv_local = key_one.shape[2] // key_width
    group = heads // kv_local
    head_width = value.shape[2] // kv_local
    scale = key_width ** (-0.5)
    positions = lax.axis_index("sp") * rows + jnp.arange(rows, dtype=jnp.int32)
    q_first = rotate(query_one, positions, heads).reshape(seqs, rows, kv_local, group, key_width)
    q_second = rotate(query_two, positions, heads).reshape(seqs, rows, kv_local, group, key_width)
    k_first = rotate(key_one, positions, kv_local).reshape(seqs, rows, kv_local * key_width)
    k_second = rotate(key_two, positions, kv_local).reshape(seqs, rows, kv_local * key_width)
    start_state = (
        jnp.full((seqs, kv_local, group, rows), NEG_BIG, jnp.float32),
        jnp.zeros((seqs, kv_local, group, rows), jnp.float32),
        jnp.zeros((seqs, kv_local, group, rows, head_width), jnp.float32),
    )
    packed = jnp.concatenate(
        [k_first, k_second, value, doc_ids.astype(jnp.bfloat16)[..., None]], axis=-1
    )
    packed = lax.all_gather(packed, "sp", axis=1, tiled=True)
    key_cols = k_first.shape[2]
    keys_one = packed[..., :key_cols]
    keys_two = packed[..., key_cols : 2 * key_cols]
    vals = packed[..., 2 * key_cols : -1]
    docs = packed[..., -1].astype(jnp.int32)
    count = keys_one.shape[1]
    step_len = math.gcd(count, 512)

    def inner(state, index):
        offset = index * step_len
        ka = lax.dynamic_slice_in_dim(keys_one, offset, step_len, 1).reshape(
            seqs, step_len, kv_local, key_width
        )
        kb = lax.dynamic_slice_in_dim(keys_two, offset, step_len, 1).reshape(
            seqs, step_len, kv_local, key_width
        )
        va = lax.dynamic_slice_in_dim(vals, offset, step_len, 1).reshape(
            seqs, step_len, kv_local, head_width
        )
        dpiece = lax.dynamic_slice_in_dim(docs, offset, step_len, 1)
        key_pos = offset + jnp.arange(step_len, dtype=jnp.int32)
        allowed = (key_pos[None, None, :] <= positions[None, :, None]) & (
            dpiece[:, None, :] == doc_ids[:, :, None]
        )
        first = online_step(state[0], q_first, ka, va, allowed, scale)
        second = online_step(state[1], q_second, kb, va, allowed, scale)
        return ((first, second), None)

    def run(state):
        return lax.scan(inner, state, jnp.arange(count // step_len))[0]

    first, second = lax.cond(
        jnp.int32(0) <= positions[rows - 1], run, lambda state: state, (start_state, start_state)
    )
    weights = lam.reshape(kv_local, group)[None, :, :, None, None]
    mixed = first[2] / first[1][..., None] - weights * (second[2] / second[1][..., None])
    meansq = jnp.mean(mixed * mixed, axis=-1, keepdims=True)
    normed_heads = mixed * lax.rsqrt(meansq + NORM_EPS) * head_gain
    heads_out = jnp.transpose(normed_heads, (0, 3, 1, 2, 4)).reshape(
        seqs * rows, heads * head_width
    )
    heads_out = heads_out.astype(jnp.bfloat16)
    proj = lax.psum_scatter(
        jnp.dot(heads_out, out_weight, preferred_element_type=jnp.float32).astype(jnp.bfloat16),
        "tp",
        scatter_dimension=0,
        tiled=True,
    ).astype(jnp.float32)
    mid = resid_in.astype(jnp.float32) + proj.reshape(resid_in.shape)
    meansq_mid = jnp.mean(mid * mid, axis=-1, keepdims=True)
    normed = (mid * lax.rsqrt(meansq_mid + NORM_EPS) * norm_gain).astype(jnp.bfloat16)
    own = normed.shape[0]
    features = normed.shape[2]
    gathered = lax.all_gather(normed, ("tp", "sp"), axis=0)
    gathered = gathered.reshape(-1, n_sp, own, rows, features)
    full_rows = jnp.transpose(gathered, (0, 2, 1, 3, 4)).reshape(-1, features)
    total_rows = n_sp * rows
    start = me * share
    taps_gate = lax.dynamic_slice_in_dim(conv_gate, start, share, 1)
    taps_value = lax.dynamic_slice_in_dim(conv_value, start, share, 1)
    up_gate = jnp.dot(full_rows, up_all[:, 0], preferred_element_type=jnp.float32)
    up_value = jnp.dot(full_rows, up_all[:, 1], preferred_element_type=jnp.float32)
    up_gate = up_gate.astype(jnp.bfloat16).reshape(seqs, total_rows, share)
    up_value = up_value.astype(jnp.bfloat16).reshape(seqs, total_rows, share)
    conv_g = depthwise(up_gate, taps_gate, docs)
    conv_v = depthwise(up_value, taps_value, docs)
    hidden = (jax.nn.silu(conv_g) * conv_v).astype(jnp.bfloat16)
    hidden = hidden.reshape(-1, own, n_sp, rows, share)
    hidden = jnp.transpose(hidden, (0, 2, 1, 3, 4)).reshape(-1, share)
    partial_down = jnp.dot(hidden, down_full, preferred_element_type=jnp.float32)
    down = lax.psum_scatter(
        partial_down.astype(jnp.bfloat16), ("tp", "sp"), scatter_dimension=0, tiled=True
    ).astype(jnp.float32)
    return (mid + down.reshape(mid.shape)).astype(jnp.bfloat16)


def solution(mesh):
    placed = (
        P(("grp", "tp"), "sp", None),
        P("grp", "sp", "tp"),
        P("grp", "sp", "tp"),
        P("grp", "sp", "tp"),
        P("grp", "sp", "tp"),
        P("grp", "sp", "tp"),
        P("tp"),
        P(),
        P("grp", "sp"),
        P("tp", None),
        P(),
        P("sp", "tp"),
        P("sp", "tp"),
        P(None, "tp"),
        P(None, "tp"),
        P("tp", "sp"),
    )
    return jax.shard_map(
        per_device,
        mesh=mesh,
        in_specs=placed,
        out_specs=P(("grp", "tp"), "sp", None),
        check_vma=False,
    )
```

```python
import functools
import math

import jax
import jax.numpy as jnp
from jax import lax
from jax.experimental import pallas as pl
from jax.experimental.pallas import tpu as pltpu
from jax.sharding import PartitionSpec as P

NEG_BIG = -1e30
NORM_EPS = 1e-06
ROPE_BASE = 500000.0


MESH = pl.DeviceIdType.MESH
VMEM = pl.BlockSpec(memory_space=pltpu.VMEM)


def greet(devices):
    barrier = pltpu.get_barrier_semaphore()
    for device in devices:
        pl.semaphore_signal(barrier, inc=1, device_id=device, device_id_type=MESH)
    pl.semaphore_wait(barrier, len(devices))


def remote(src, dst, send_sem, recv_sem, device):
    return pltpu.make_async_remote_copy(
        src_ref=src,
        dst_ref=dst,
        send_sem=send_sem,
        recv_sem=recv_sem,
        device_id=device,
        device_id_type=MESH,
    )


def partners():
    at = lax.axis_index("tp")
    return at, at + 1 - 2 * lax.rem(at, 2), lax.rem(at + 2, 4)


def spread_kernel(n, own_ref, out_ref, send_sem, recv_sem):
    me = lax.axis_index("sp")
    peers = [lax.rem(me + shift, n) for shift in range(1, n)]
    greet([{"sp": peer} for peer in peers])
    copies = []
    for k, peer in enumerate(peers):
        copy = remote(
            own_ref, out_ref.at[:, me], send_sem.at[k], recv_sem.at[k], {"sp": peer}
        )
        copy.start()
        copies.append(copy)
    out_ref[:, me] = own_ref[...]
    for copy in copies:
        copy.wait_recv()
    for copy in copies:
        copy.wait_send()


def gather_sp(own):
    n = lax.axis_size("sp")
    if n > 8:
        return lax.all_gather(own, "sp", axis=1, tiled=True)
    outer, rows, width = own.shape
    out = pl.pallas_call(
        functools.partial(spread_kernel, n),
        out_shape=jax.ShapeDtypeStruct((outer, n, rows, width), own.dtype),
        in_specs=[VMEM],
        out_specs=VMEM,
        scratch_shapes=[pltpu.SemaphoreType.DMA((n - 1,)), pltpu.SemaphoreType.DMA((n - 1,))],
        compiler_params=pltpu.CompilerParams(collective_id=1, has_side_effects=True),
        cost_estimate=pl.CostEstimate(flops=0, bytes_accessed=30_000_000, transcendentals=0),
        name="gather_sp",
    )(own)
    return out.reshape(outer, n * rows, width)


def rows_kernel(n, own_ref, out_ref, z_send, z_recv, x_send, x_recv, c_send, c_recv):
    me = lax.axis_index("sp")
    tp, near, far = partners()
    greet([{"tp": near}, {"tp": far}] + [{"sp": lax.rem(me + k, n)} for k in range(1, n)])
    sources = [lax.rem(me - k + n, n) for k in range(n)]
    z_copies = []
    for k in range(1, n):
        copy = remote(
            own_ref,
            out_ref.at[tp, me],
            z_send.at[k - 1],
            z_recv.at[k - 1],
            {"sp": lax.rem(me + k, n)},
        )
        z_copies.append(copy)

    def along(owner, k, send, recv, device):
        block = out_ref.at[owner, sources[k]]
        return remote(block, block, send, recv, device)

    x_copies = [remote(own_ref, out_ref.at[tp, me], x_send.at[0], x_recv.at[0], {"tp": far})]
    c_copies = [remote(own_ref, out_ref.at[tp, me], c_send.at[0], c_recv.at[0], {"tp": near})]
    for k in range(1, n):
        x_copies.append(along(tp, k, x_send.at[k], x_recv.at[k], {"tp": far}))
        c_copies.append(along(tp, k, c_send.at[k], c_recv.at[k], {"tp": near}))
    f_copies = [along(far, k, c_send.at[n + k], c_recv.at[n + k], {"tp": near}) for k in range(n)]
    x_copies[0].start()
    for copy in z_copies:
        copy.start()
    c_copies[0].start()
    out_ref[tp, me] = own_ref[...]
    for k in range(1, n):
        z_copies[k - 1].wait_recv()
        x_copies[k].start()
        c_copies[k].start()
    for k in range(n):
        x_copies[k].wait_recv()
        f_copies[k].start()
    for copy in c_copies + f_copies:
        copy.wait_recv()
    for copy in z_copies + x_copies + c_copies + f_copies:
        copy.wait_send()


def gather_rows(own):
    n, wide = lax.axis_size("sp"), lax.axis_size("tp")
    if n > 8 or wide != 4:
        out = lax.all_gather(own, ("tp", "sp"), axis=0)
        return out.reshape((wide, n) + own.shape)
    dma = pltpu.SemaphoreType.DMA
    return pl.pallas_call(
        functools.partial(rows_kernel, n),
        out_shape=jax.ShapeDtypeStruct((wide, n) + own.shape, own.dtype),
        in_specs=[VMEM],
        out_specs=VMEM,
        scratch_shapes=[
            dma((n - 1,)),
            dma((n - 1,)),
            dma((n,)),
            dma((n,)),
            dma((2 * n,)),
            dma((2 * n,)),
        ],
        compiler_params=pltpu.CompilerParams(collective_id=2, has_side_effects=True),
        cost_estimate=pl.CostEstimate(flops=0, bytes_accessed=90_000_000, transcendentals=0),
        name="gather_rows",
    )(own)


def reduce_kernel(
    n, chunks, part_ref, base_ref, out_ref, got_c, sum_c, got_x, sum_x, got_z,
    c_send, c_recv, x_send, x_recv, z_send, z_recv,
):
    tp, near, far = partners()
    low, high = lax.rem(tp, 2), tp // 2
    shifts = range(1, n)
    me = lax.axis_index("sp") if n > 1 else 0
    greet([{"tp": near}, {"tp": far}] + [{"sp": lax.rem(me + k, n)} for k in shifts])
    width = part_ref.shape[-1] // chunks
    cols = [pl.ds(i * width, width) for i in range(chunks)]
    c_copies, x_copies, z_copies = [], [], []
    for i in range(chunks):
        copy = remote(
            part_ref.at[:, 1 - low, :, :, cols[i]],
            got_c.at[i],
            c_send.at[i],
            c_recv.at[i],
            {"tp": near},
        )
        copy.start()
        c_copies.append(copy)
    for i in range(chunks):
        c_copies[i].wait_recv()
        mine = part_ref[:, low, :, :, cols[i]].astype(jnp.float32)
        sum_c[i] = (mine + got_c[i].astype(jnp.float32)).astype(sum_c.dtype)
        copy = remote(
            sum_c.at[i, 1 - high], got_x.at[i], x_send.at[i], x_recv.at[i], {"tp": far}
        )
        copy.start()
        x_copies.append(copy)
    for i in range(chunks):
        x_copies[i].wait_recv()
        both = sum_c[i, high].astype(jnp.float32) + got_x[i].astype(jnp.float32)
        sum_x[i] = both.astype(sum_x.dtype)
        for k in shifts:
            peer = lax.rem(me + k, n)
            copy = remote(
                sum_x.at[i, peer],
                got_z.at[i, k - 1],
                z_send.at[i, k - 1],
                z_recv.at[i, k - 1],
                {"sp": peer},
            )
            copy.start()
            z_copies.append(copy)
    for i in range(chunks):
        total = sum_x[i, me].astype(jnp.float32)
        for k in shifts:
            z_copies[i * (n - 1) + k - 1].wait_recv()
            total = total + got_z[i, k - 1].astype(jnp.float32)
        out_ref[:, cols[i]] = (base_ref[:, cols[i]] + total).astype(out_ref.dtype)
    for copy in c_copies + x_copies + z_copies:
        copy.wait_send()


def reduce_rows(part, base, dtype, over_sp):
    wide, n = part.shape[:2]
    if n > 8 or wide != 4 or part.size > 8_000_000:
        axes = ("tp", "sp") if over_sp else "tp"
        flat = part.reshape(-1, part.shape[-1])
        total = lax.psum_scatter(flat, axes, scatter_dimension=0, tiled=True)
        return (base + total.astype(jnp.float32)).astype(dtype)
    rows, columns = part.shape[2:]
    chunks = 4 if columns % 512 == 0 else 1
    width = columns // chunks
    dma = pltpu.SemaphoreType.DMA
    zs = max(n - 1, 1)
    return pl.pallas_call(
        functools.partial(reduce_kernel, n, chunks),
        out_shape=jax.ShapeDtypeStruct((rows, columns), dtype),
        in_specs=[VMEM, VMEM],
        out_specs=VMEM,
        scratch_shapes=[
            pltpu.VMEM((chunks, 2, n, rows, width), part.dtype),
            pltpu.VMEM((chunks, 2, n, rows, width), part.dtype),
            pltpu.VMEM((chunks, n, rows, width), part.dtype),
            pltpu.VMEM((chunks, n, rows, width), part.dtype),
            pltpu.VMEM((chunks, zs, rows, width), part.dtype),
            dma((chunks,)),
            dma((chunks,)),
            dma((chunks,)),
            dma((chunks,)),
            dma((chunks, zs)),
            dma((chunks, zs)),
        ],
        compiler_params=pltpu.CompilerParams(
            collective_id=3 if over_sp else 4, has_side_effects=True
        ),
        cost_estimate=pl.CostEstimate(flops=0, bytes_accessed=60_000_000, transcendentals=0),
        name="reduce_all" if over_sp else "reduce_tp",
    )(part.reshape(2, 2, n, rows, columns), base)


def rotate(block, positions, heads):
    entries = block.astype(jnp.float32).reshape(block.shape[:-1] + (heads, -1))
    width = entries.shape[-1]
    half = width // 2
    freqs = ROPE_BASE ** (-jnp.arange(half, dtype=jnp.float32) * 2.0 / width)
    angles = positions.astype(jnp.float32)[:, None] * freqs[None, :]
    cosine = jnp.cos(angles)[:, None, :]
    sine = jnp.sin(angles)[:, None, :]
    first = entries[..., :half]
    second = entries[..., half:]
    turned = jnp.concatenate(
        [first * cosine - second * sine, second * cosine + first * sine], axis=-1
    )
    return turned.astype(jnp.bfloat16)


def depthwise(current, taps, docs):
    shown = current.astype(jnp.float32)
    total = taps[2] * shown
    for back in (1, 2):
        moved = jnp.pad(shown, ((0, 0), (back, 0), (0, 0)))[:, : shown.shape[1]]
        moved_docs = jnp.pad(docs, ((0, 0), (back, 0)), constant_values=-1)[:, : docs.shape[1]]
        total = total + jnp.where((moved_docs == docs)[..., None], taps[2 - back] * moved, 0.0)
    return total


def cyclic(array, axis, by):
    length = lax.axis_size(axis)
    return lax.ppermute(array, axis, [(i, (i + by) % length) for i in range(length)])


def exchange(pieces):
    count = lax.axis_size("sp")
    copies = lax.axis_size("grp")
    me = lax.axis_index("sp")
    mine = lax.axis_index("grp")
    if count > 8:
        return lax.all_to_all(pieces, "sp", 0, 0)
    shared = pieces.reshape(count, copies, pieces.shape[1] // copies, *pieces.shape[2:])
    parts = []
    for shift in range(1, count):
        dest = lax.rem(me + shift, count)
        part = lax.dynamic_slice(
            shared, (dest, mine) + (0,) * (shared.ndim - 2), (1, 1) + shared.shape[2:]
        )[0, 0]
        with jax.named_scope("along_sp"):
            parts.append(cyclic(part, "sp", shift))
    got = [jnp.stack(parts, axis=0)]
    for turn in range(1, copies):
        with jax.named_scope("along_grp"):
            got.append(cyclic(got[0], "grp", turn))
    got = jnp.stack(got, axis=0)
    order = [lax.rem(mine - share + copies, copies) for share in range(copies)]
    got = jnp.stack([lax.dynamic_index_in_dim(got, at, 0, keepdims=False) for at in order], 1)
    got = got.reshape((count - 1,) + pieces.shape[1:])
    stacked = jnp.concatenate([lax.dynamic_index_in_dim(pieces, me, 0), got], axis=0)
    return jnp.stack(
        [
            lax.dynamic_index_in_dim(stacked, lax.rem(me - source + count, count), 0, keepdims=False)
            for source in range(count)
        ],
        axis=0,
    )


def online_step(state, queries, keys, vals, allowed, scale):
    peak, total, accum = state
    scores = (
        jnp.einsum("sqhgd,skhd->shgqk", queries, keys, preferred_element_type=jnp.float32) * scale
    )
    mask = allowed[:, None, None]
    scores = jnp.where(mask, scores, NEG_BIG)
    new_peak = jnp.maximum(peak, jnp.max(scores, axis=-1))
    expd = jnp.where(mask, jnp.exp(scores - new_peak[..., None]), 0.0)
    fade = jnp.exp(peak - new_peak)
    new_total = total * fade + jnp.sum(expd, axis=-1)
    update = jnp.einsum(
        "shgqk,skhd->shgqd", expd.astype(jnp.bfloat16), vals, preferred_element_type=jnp.float32
    )
    return (new_peak, new_total, accum * fade[..., None] + update)


def per_device(
    resid_in,
    query_one,
    key_one,
    query_two,
    key_two,
    value,
    lam,
    head_gain,
    doc_ids,
    out_weight,
    norm_gain,
    gate_weight,
    value_weight,
    conv_gate,
    conv_value,
    down_weight,
):
    n_sp = lax.axis_size("sp")
    me = lax.axis_index("sp")
    depth, width = gate_weight.shape
    share = width // n_sp
    up_pieces = jnp.stack([gate_weight, value_weight], axis=1).reshape(depth, 2, n_sp, share)
    up_all = exchange(jnp.transpose(up_pieces, (2, 0, 1, 3)))
    down_all = exchange(down_weight.reshape(n_sp, share, down_weight.shape[1]))
    up_all = up_all.reshape(n_sp * depth, 2, share)
    down_full = jnp.transpose(down_all, (1, 0, 2)).reshape(share, -1)
    seqs = query_one.shape[0]
    rows = query_one.shape[1]
    heads = lam.shape[0]
    key_width = query_one.shape[2] // heads
    kv_local = key_one.shape[2] // key_width
    group = heads // kv_local
    head_width = value.shape[2] // kv_local
    scale = key_width ** (-0.5)
    positions = lax.axis_index("sp") * rows + jnp.arange(rows, dtype=jnp.int32)
    q_first = rotate(query_one, positions, heads).reshape(seqs, rows, kv_local, group, key_width)
    q_second = rotate(query_two, positions, heads).reshape(seqs, rows, kv_local, group, key_width)
    k_first = rotate(key_one, positions, kv_local).reshape(seqs, rows, kv_local * key_width)
    k_second = rotate(key_two, positions, kv_local).reshape(seqs, rows, kv_local * key_width)
    start_state = (
        jnp.full((seqs, kv_local, group, rows), NEG_BIG, jnp.float32),
        jnp.zeros((seqs, kv_local, group, rows), jnp.float32),
        jnp.zeros((seqs, kv_local, group, rows, head_width), jnp.float32),
    )
    packed = jnp.concatenate(
        [k_first, k_second, value, doc_ids.astype(jnp.bfloat16)[..., None]], axis=-1
    )
    packed = gather_sp(packed)
    key_cols = k_first.shape[2]
    keys_one = packed[..., :key_cols]
    keys_two = packed[..., key_cols : 2 * key_cols]
    vals = packed[..., 2 * key_cols : -1]
    docs = packed[..., -1].astype(jnp.int32)
    count = keys_one.shape[1]
    step_len = math.gcd(count, 512)

    def inner(state, index):
        offset = index * step_len
        ka = lax.dynamic_slice_in_dim(keys_one, offset, step_len, 1).reshape(
            seqs, step_len, kv_local, key_width
        )
        kb = lax.dynamic_slice_in_dim(keys_two, offset, step_len, 1).reshape(
            seqs, step_len, kv_local, key_width
        )
        va = lax.dynamic_slice_in_dim(vals, offset, step_len, 1).reshape(
            seqs, step_len, kv_local, head_width
        )
        dpiece = lax.dynamic_slice_in_dim(docs, offset, step_len, 1)
        key_pos = offset + jnp.arange(step_len, dtype=jnp.int32)
        allowed = (key_pos[None, None, :] <= positions[None, :, None]) & (
            dpiece[:, None, :] == doc_ids[:, :, None]
        )
        first = online_step(state[0], q_first, ka, va, allowed, scale)
        second = online_step(state[1], q_second, kb, va, allowed, scale)
        return ((first, second), None)

    def run(state):
        return lax.scan(inner, state, jnp.arange(count // step_len))[0]

    first, second = lax.cond(
        jnp.int32(0) <= positions[rows - 1], run, lambda state: state, (start_state, start_state)
    )
    weights = lam.reshape(kv_local, group)[None, :, :, None, None]
    mixed = first[2] / first[1][..., None] - weights * (second[2] / second[1][..., None])
    meansq = jnp.mean(mixed * mixed, axis=-1, keepdims=True)
    normed_heads = mixed * lax.rsqrt(meansq + NORM_EPS) * head_gain
    heads_out = jnp.transpose(normed_heads, (0, 3, 1, 2, 4)).reshape(
        seqs * rows, heads * head_width
    )
    heads_out = heads_out.astype(jnp.bfloat16)
    own = resid_in.shape[0]
    features = resid_in.shape[2]
    proj = jnp.dot(heads_out, out_weight, preferred_element_type=jnp.float32).astype(jnp.bfloat16)
    mid = reduce_rows(
        proj.reshape(-1, 1, own * rows, features),
        resid_in.astype(jnp.float32).reshape(own * rows, features),
        jnp.float32,
        False,
    )
    meansq_mid = jnp.mean(mid * mid, axis=-1, keepdims=True)
    normed = (mid * lax.rsqrt(meansq_mid + NORM_EPS) * norm_gain).astype(jnp.bfloat16)
    gathered = gather_rows(normed).reshape(-1, n_sp, own, rows, features)
    full_rows = jnp.transpose(gathered, (0, 2, 1, 3, 4)).reshape(-1, features)
    total_rows = n_sp * rows
    start = me * share
    taps_gate = lax.dynamic_slice_in_dim(conv_gate, start, share, 1)
    taps_value = lax.dynamic_slice_in_dim(conv_value, start, share, 1)
    up_gate = jnp.dot(full_rows, up_all[:, 0], preferred_element_type=jnp.float32)
    up_value = jnp.dot(full_rows, up_all[:, 1], preferred_element_type=jnp.float32)
    up_gate = up_gate.astype(jnp.bfloat16).reshape(seqs, total_rows, share)
    up_value = up_value.astype(jnp.bfloat16).reshape(seqs, total_rows, share)
    conv_g = depthwise(up_gate, taps_gate, docs)
    conv_v = depthwise(up_value, taps_value, docs)
    hidden = (jax.nn.silu(conv_g) * conv_v).astype(jnp.bfloat16)
    hidden = hidden.reshape(-1, own, n_sp, rows, share)
    hidden = jnp.transpose(hidden, (0, 2, 1, 3, 4)).reshape(-1, share)
    partial_down = jnp.dot(hidden, down_full, preferred_element_type=jnp.float32)
    partial_down = partial_down.astype(jnp.bfloat16).reshape(-1, n_sp, own * rows, features)
    return reduce_rows(partial_down, mid, jnp.bfloat16, True).reshape(resid_in.shape)


def solution(mesh):
    placed = (
        P(("grp", "tp"), "sp", None),
        P("grp", "sp", "tp"),
        P("grp", "sp", "tp"),
        P("grp", "sp", "tp"),
        P("grp", "sp", "tp"),
        P("grp", "sp", "tp"),
        P("tp"),
        P(),
        P("grp", "sp"),
        P("tp", None),
        P(),
        P("sp", "tp"),
        P("sp", "tp"),
        P(None, "tp"),
        P(None, "tp"),
        P("tp", "sp"),
    )
    return jax.shard_map(
        per_device,
        mesh=mesh,
        in_specs=placed,
        out_specs=P(("grp", "tp"), "sp", None),
        check_vma=False,
    )
```

```python
import functools
import math

import jax
import jax.numpy as jnp
from jax import lax
from jax.experimental import pallas as pl
from jax.experimental.pallas import tpu as pltpu
from jax.sharding import PartitionSpec as P

NEG_BIG = -1e30
NORM_EPS = 1e-06
ROPE_BASE = 500000.0


MESH = pl.DeviceIdType.MESH
VMEM = pl.BlockSpec(memory_space=pltpu.VMEM)


def greet(devices):
    barrier = pltpu.get_barrier_semaphore()
    for device in devices:
        pl.semaphore_signal(barrier, inc=1, device_id=device, device_id_type=MESH)
    pl.semaphore_wait(barrier, len(devices))


def remote(src, dst, send_sem, recv_sem, device):
    return pltpu.make_async_remote_copy(
        src_ref=src,
        dst_ref=dst,
        send_sem=send_sem,
        recv_sem=recv_sem,
        device_id=device,
        device_id_type=MESH,
    )


def partners():
    at = lax.axis_index("tp")
    return at, at + 1 - 2 * lax.rem(at, 2), lax.rem(at + 2, 4)


def spread_kernel(n, own_ref, out_ref, send_sem, recv_sem):
    me = lax.axis_index("sp")
    peers = [lax.rem(me + shift, n) for shift in range(1, n)]
    greet([{"sp": peer} for peer in peers])
    copies = []
    for k, peer in enumerate(peers):
        copy = remote(
            own_ref, out_ref.at[:, me], send_sem.at[k], recv_sem.at[k], {"sp": peer}
        )
        copy.start()
        copies.append(copy)
    out_ref[:, me] = own_ref[...]
    for copy in copies:
        copy.wait_recv()
    for copy in copies:
        copy.wait_send()


def gather_sp(own):
    n = lax.axis_size("sp")
    if n > 8:
        return lax.all_gather(own, "sp", axis=1, tiled=True)
    outer, rows, width = own.shape
    out = pl.pallas_call(
        functools.partial(spread_kernel, n),
        out_shape=jax.ShapeDtypeStruct((outer, n, rows, width), own.dtype),
        in_specs=[VMEM],
        out_specs=VMEM,
        scratch_shapes=[pltpu.SemaphoreType.DMA((n - 1,)), pltpu.SemaphoreType.DMA((n - 1,))],
        compiler_params=pltpu.CompilerParams(collective_id=1, has_side_effects=True),
        cost_estimate=pl.CostEstimate(flops=0, bytes_accessed=30_000_000, transcendentals=0),
        name="gather_sp",
    )(own)
    return out.reshape(outer, n * rows, width)


def rows_kernel(n, own_ref, out_ref, z_send, z_recv, x_send, x_recv, c_send, c_recv):
    me = lax.axis_index("sp")
    tp, near, far = partners()
    greet([{"tp": near}, {"tp": far}] + [{"sp": lax.rem(me + k, n)} for k in range(1, n)])
    sources = [lax.rem(me - k + n, n) for k in range(n)]
    z_copies = []
    for k in range(1, n):
        copy = remote(
            own_ref,
            out_ref.at[tp, me],
            z_send.at[k - 1],
            z_recv.at[k - 1],
            {"sp": lax.rem(me + k, n)},
        )
        z_copies.append(copy)

    def along(owner, k, send, recv, device):
        block = out_ref.at[owner, sources[k]]
        return remote(block, block, send, recv, device)

    x_copies = [remote(own_ref, out_ref.at[tp, me], x_send.at[0], x_recv.at[0], {"tp": far})]
    c_copies = [remote(own_ref, out_ref.at[tp, me], c_send.at[0], c_recv.at[0], {"tp": near})]
    for k in range(1, n):
        x_copies.append(along(tp, k, x_send.at[k], x_recv.at[k], {"tp": far}))
        c_copies.append(along(tp, k, c_send.at[k], c_recv.at[k], {"tp": near}))
    f_copies = [along(far, k, c_send.at[n + k], c_recv.at[n + k], {"tp": near}) for k in range(n)]
    x_copies[0].start()
    for copy in z_copies:
        copy.start()
    c_copies[0].start()
    out_ref[tp, me] = own_ref[...]
    for k in range(1, n):
        z_copies[k - 1].wait_recv()
        x_copies[k].start()
        c_copies[k].start()
    for k in range(n):
        x_copies[k].wait_recv()
        f_copies[k].start()
    for copy in c_copies + f_copies:
        copy.wait_recv()
    for copy in z_copies + x_copies + c_copies + f_copies:
        copy.wait_send()


def gather_rows(own):
    n, wide = lax.axis_size("sp"), lax.axis_size("tp")
    if n > 8 or wide != 4:
        out = lax.all_gather(own, ("tp", "sp"), axis=0)
        return out.reshape((wide, n) + own.shape)
    dma = pltpu.SemaphoreType.DMA
    return pl.pallas_call(
        functools.partial(rows_kernel, n),
        out_shape=jax.ShapeDtypeStruct((wide, n) + own.shape, own.dtype),
        in_specs=[VMEM],
        out_specs=VMEM,
        scratch_shapes=[
            dma((n - 1,)),
            dma((n - 1,)),
            dma((n,)),
            dma((n,)),
            dma((2 * n,)),
            dma((2 * n,)),
        ],
        compiler_params=pltpu.CompilerParams(collective_id=2, has_side_effects=True),
        cost_estimate=pl.CostEstimate(flops=0, bytes_accessed=90_000_000, transcendentals=0),
        name="gather_rows",
    )(own)


def reduce_kernel(
    n, chunks, part_ref, base_ref, out_ref, got_c, sum_c, got_x, sum_x, got_z,
    c_send, c_recv, x_send, x_recv, z_send, z_recv,
):
    tp, near, far = partners()
    low, high = lax.rem(tp, 2), tp // 2
    shifts = range(1, n)
    me = lax.axis_index("sp") if n > 1 else 0
    greet([{"tp": near}, {"tp": far}] + [{"sp": lax.rem(me + k, n)} for k in shifts])
    width = part_ref.shape[-1] // chunks
    cols = [pl.ds(i * width, width) for i in range(chunks)]
    c_copies, x_copies, z_copies = [], [], []
    for i in range(chunks):
        copy = remote(
            part_ref.at[:, 1 - low, :, :, cols[i]],
            got_c.at[i],
            c_send.at[i],
            c_recv.at[i],
            {"tp": near},
        )
        copy.start()
        c_copies.append(copy)
    for i in range(chunks):
        c_copies[i].wait_recv()
        mine = part_ref[:, low, :, :, cols[i]].astype(jnp.float32)
        sum_c[i] = (mine + got_c[i].astype(jnp.float32)).astype(sum_c.dtype)
        copy = remote(
            sum_c.at[i, 1 - high], got_x.at[i], x_send.at[i], x_recv.at[i], {"tp": far}
        )
        copy.start()
        x_copies.append(copy)
    for i in range(chunks):
        x_copies[i].wait_recv()
        both = sum_c[i, high].astype(jnp.float32) + got_x[i].astype(jnp.float32)
        sum_x[i] = both.astype(sum_x.dtype)
        for k in shifts:
            peer = lax.rem(me + k, n)
            copy = remote(
                sum_x.at[i, peer],
                got_z.at[i, k - 1],
                z_send.at[i, k - 1],
                z_recv.at[i, k - 1],
                {"sp": peer},
            )
            copy.start()
            z_copies.append(copy)
    for i in range(chunks):
        total = sum_x[i, me].astype(jnp.float32)
        for k in shifts:
            z_copies[i * (n - 1) + k - 1].wait_recv()
            total = total + got_z[i, k - 1].astype(jnp.float32)
        out_ref[:, cols[i]] = (base_ref[:, cols[i]] + total).astype(out_ref.dtype)
    for copy in c_copies + x_copies + z_copies:
        copy.wait_send()


def reduce_rows(part, base, dtype, over_sp):
    wide, n = part.shape[:2]
    if n > 8 or wide != 4 or part.size > 8_000_000:
        axes = ("tp", "sp") if over_sp else "tp"
        flat = part.reshape(-1, part.shape[-1])
        total = lax.psum_scatter(flat, axes, scatter_dimension=0, tiled=True)
        return (base + total.astype(jnp.float32)).astype(dtype)
    rows, columns = part.shape[2:]
    chunks = 4 if columns % 512 == 0 else 1
    width = columns // chunks
    dma = pltpu.SemaphoreType.DMA
    zs = max(n - 1, 1)
    return pl.pallas_call(
        functools.partial(reduce_kernel, n, chunks),
        out_shape=jax.ShapeDtypeStruct((rows, columns), dtype),
        in_specs=[VMEM, VMEM],
        out_specs=VMEM,
        scratch_shapes=[
            pltpu.VMEM((chunks, 2, n, rows, width), part.dtype),
            pltpu.VMEM((chunks, 2, n, rows, width), part.dtype),
            pltpu.VMEM((chunks, n, rows, width), part.dtype),
            pltpu.VMEM((chunks, n, rows, width), part.dtype),
            pltpu.VMEM((chunks, zs, rows, width), part.dtype),
            dma((chunks,)),
            dma((chunks,)),
            dma((chunks,)),
            dma((chunks,)),
            dma((chunks, zs)),
            dma((chunks, zs)),
        ],
        compiler_params=pltpu.CompilerParams(
            collective_id=3 if over_sp else 4, has_side_effects=True
        ),
        cost_estimate=pl.CostEstimate(flops=0, bytes_accessed=60_000_000, transcendentals=0),
        name="reduce_all" if over_sp else "reduce_tp",
    )(part.reshape(2, 2, n, rows, columns), base)


def rotate(block, positions, heads):
    columns = block.shape[-1]
    width = columns // heads
    half = width // 2
    at = jnp.arange(columns, dtype=jnp.int32)
    freqs = ROPE_BASE ** (-(at % half).astype(jnp.float32) * 2.0 / width)
    angles = positions.astype(jnp.float32)[:, None] * freqs[None, :]
    source = jnp.where(at % width < half, at + half, at - half)
    sign = jnp.where(at % width < half, -1.0, 1.0)
    turn = jnp.where(at[:, None] == source[None, :], sign[None, :], 0.0).astype(jnp.bfloat16)
    flat = block.reshape(-1, columns)
    other = jnp.dot(flat, turn, preferred_element_type=jnp.float32).reshape(block.shape)
    turned = block.astype(jnp.float32) * jnp.cos(angles) + other * jnp.sin(angles)
    return turned.astype(jnp.bfloat16)


def depthwise(current, taps, docs):
    shown = current.astype(jnp.float32)
    total = taps[2] * shown
    for back in (1, 2):
        moved = jnp.pad(shown, ((0, 0), (back, 0), (0, 0)))[:, : shown.shape[1]]
        moved_docs = jnp.pad(docs, ((0, 0), (back, 0)), constant_values=-1)[:, : docs.shape[1]]
        total = total + jnp.where((moved_docs == docs)[..., None], taps[2 - back] * moved, 0.0)
    return total


def cyclic(array, axis, by):
    length = lax.axis_size(axis)
    return lax.ppermute(array, axis, [(i, (i + by) % length) for i in range(length)])


def exchange(piece, whole):
    count = lax.axis_size("sp")
    copies = lax.axis_size("grp")
    me = lax.axis_index("sp")
    mine = lax.axis_index("grp")
    if count > 8:
        pieces = jnp.stack([whole(dest) for dest in range(count)], axis=0)
        return lax.all_to_all(pieces, "sp", 0, 0)
    parts = []
    for shift in range(1, count):
        part = piece(lax.rem(me + shift, count), mine)
        parts.append(cyclic(part, "sp", shift))
    got = [jnp.stack(parts, axis=0)]
    for turn in range(1, copies):
        got.append(cyclic(got[0], "grp", turn))
    got = jnp.stack(got, axis=1)
    held = whole(me)
    held = jnp.broadcast_to(held[None], (1,) + held.shape)
    order = [lax.rem(mine - share + copies, copies) for share in range(copies)]
    out = []
    for source in range(count):
        shift = lax.rem(me - source + count, count)
        there = lax.max(shift - 1, 0)
        shares = [
            lax.dynamic_slice(got, (there, at) + (0,) * (got.ndim - 2), (1, 1) + got.shape[2:])[0]
            for at in order
        ]
        out.append(jnp.where(shift == 0, held, jnp.concatenate(shares, axis=0)[None]))
    return jnp.concatenate(out, axis=0)


def online_step(state, queries, keys, vals, allowed, scale):
    peak, total, accum = state
    scores = (
        jnp.einsum("sqhgd,skhd->shgqk", queries, keys, preferred_element_type=jnp.float32) * scale
    )
    mask = allowed[:, None, None]
    scores = jnp.where(mask, scores, NEG_BIG)
    new_peak = jnp.maximum(peak, jnp.max(scores, axis=-1))
    expd = jnp.where(mask, jnp.exp(scores - new_peak[..., None]), 0.0)
    fade = jnp.exp(peak - new_peak)
    new_total = total * fade + jnp.sum(expd, axis=-1)
    update = jnp.einsum(
        "shgqk,skhd->shgqd", expd.astype(jnp.bfloat16), vals, preferred_element_type=jnp.float32
    )
    return (new_peak, new_total, accum * fade[..., None] + update)


def per_device(
    resid_in,
    query_one,
    key_one,
    query_two,
    key_two,
    value,
    lam,
    head_gain,
    doc_ids,
    out_weight,
    norm_gain,
    gate_weight,
    value_weight,
    conv_gate,
    conv_value,
    down_weight,
):
    n_sp = lax.axis_size("sp")
    me = lax.axis_index("sp")
    depth, width = gate_weight.shape
    share = width // n_sp
    copies = lax.axis_size("grp")

    def cut(weight, row, column, size):
        return lax.dynamic_slice(weight, (row, column), size)

    def up_piece(dest, part):
        size = (depth // copies, share)
        row, column = part * size[0], dest * share
        return jnp.stack([cut(gate_weight, row, column, size), cut(value_weight, row, column, size)])

    def up_whole(dest):
        return jnp.stack([up_piece(dest, part) for part in range(copies)])

    def down_piece(dest, part):
        size = (share // copies, down_weight.shape[1])
        return cut(down_weight, dest * share + part * size[0], 0, size)

    def down_whole(dest):
        return jnp.stack([down_piece(dest, part) for part in range(copies)])

    up_all = exchange(up_piece, up_whole)
    down_all = exchange(down_piece, down_whole)
    gate_all = up_all[:, :, 0].reshape(-1, share)
    value_all = up_all[:, :, 1].reshape(-1, share)
    down_full = jnp.transpose(down_all, (1, 2, 0, 3)).reshape(share, -1)
    seqs = query_one.shape[0]
    rows = query_one.shape[1]
    heads = lam.shape[0]
    key_width = query_one.shape[2] // heads
    kv_local = key_one.shape[2] // key_width
    group = heads // kv_local
    head_width = value.shape[2] // kv_local
    scale = key_width ** (-0.5)
    positions = lax.axis_index("sp") * rows + jnp.arange(rows, dtype=jnp.int32)
    q_first = rotate(query_one, positions, heads).reshape(seqs, rows, kv_local, group, key_width)
    q_second = rotate(query_two, positions, heads).reshape(seqs, rows, kv_local, group, key_width)
    k_first = rotate(key_one, positions, kv_local).reshape(seqs, rows, kv_local * key_width)
    k_second = rotate(key_two, positions, kv_local).reshape(seqs, rows, kv_local * key_width)
    start_state = (
        jnp.full((seqs, kv_local, group, rows), NEG_BIG, jnp.float32),
        jnp.zeros((seqs, kv_local, group, rows), jnp.float32),
        jnp.zeros((seqs, kv_local, group, rows, head_width), jnp.float32),
    )
    packed = jnp.concatenate(
        [k_first, k_second, value, doc_ids.astype(jnp.bfloat16)[..., None]], axis=-1
    )
    packed = gather_sp(packed)
    key_cols = k_first.shape[2]
    keys_one = packed[..., :key_cols]
    keys_two = packed[..., key_cols : 2 * key_cols]
    vals = packed[..., 2 * key_cols : -1]
    docs = packed[..., -1].astype(jnp.int32)
    count = keys_one.shape[1]
    step_len = math.gcd(count, 512)

    def inner(state, index):
        offset = index * step_len
        ka = lax.dynamic_slice_in_dim(keys_one, offset, step_len, 1).reshape(
            seqs, step_len, kv_local, key_width
        )
        kb = lax.dynamic_slice_in_dim(keys_two, offset, step_len, 1).reshape(
            seqs, step_len, kv_local, key_width
        )
        va = lax.dynamic_slice_in_dim(vals, offset, step_len, 1).reshape(
            seqs, step_len, kv_local, head_width
        )
        dpiece = lax.dynamic_slice_in_dim(docs, offset, step_len, 1)
        key_pos = offset + jnp.arange(step_len, dtype=jnp.int32)
        allowed = (key_pos[None, None, :] <= positions[None, :, None]) & (
            dpiece[:, None, :] == doc_ids[:, :, None]
        )
        first = online_step(state[0], q_first, ka, va, allowed, scale)
        second = online_step(state[1], q_second, kb, va, allowed, scale)
        return ((first, second), None)

    def run(state):
        return lax.scan(inner, state, jnp.arange(count // step_len))[0]

    first, second = lax.cond(
        jnp.int32(0) <= positions[rows - 1], run, lambda state: state, (start_state, start_state)
    )
    weights = lam.reshape(kv_local, group)[None, :, :, None, None]
    mixed = first[2] / first[1][..., None] - weights * (second[2] / second[1][..., None])
    meansq = jnp.mean(mixed * mixed, axis=-1, keepdims=True)
    normed_heads = mixed * lax.rsqrt(meansq + NORM_EPS) * head_gain
    heads_out = jnp.transpose(normed_heads, (0, 3, 1, 2, 4)).reshape(
        seqs * rows, heads * head_width
    )
    heads_out = heads_out.astype(jnp.bfloat16)
    own = resid_in.shape[0]
    features = resid_in.shape[2]
    proj = jnp.dot(heads_out, out_weight, preferred_element_type=jnp.float32).astype(jnp.bfloat16)
    mid = reduce_rows(
        proj.reshape(-1, 1, own * rows, features),
        resid_in.astype(jnp.float32).reshape(own * rows, features),
        jnp.float32,
        False,
    )
    meansq_mid = jnp.mean(mid * mid, axis=-1, keepdims=True)
    normed = (mid * lax.rsqrt(meansq_mid + NORM_EPS) * norm_gain).astype(jnp.bfloat16)
    gathered = gather_rows(normed).reshape(-1, n_sp, own, rows, features)
    full_rows = jnp.transpose(gathered, (0, 2, 1, 3, 4)).reshape(-1, features)
    total_rows = n_sp * rows
    start = me * share
    taps_gate = lax.dynamic_slice_in_dim(conv_gate, start, share, 1)
    taps_value = lax.dynamic_slice_in_dim(conv_value, start, share, 1)
    up_gate = jnp.dot(full_rows, gate_all, preferred_element_type=jnp.float32)
    up_value = jnp.dot(full_rows, value_all, preferred_element_type=jnp.float32)
    up_gate = up_gate.astype(jnp.bfloat16).reshape(seqs, total_rows, share)
    up_value = up_value.astype(jnp.bfloat16).reshape(seqs, total_rows, share)
    conv_g = depthwise(up_gate, taps_gate, docs)
    conv_v = depthwise(up_value, taps_value, docs)
    hidden = (jax.nn.silu(conv_g) * conv_v).astype(jnp.bfloat16)
    hidden = hidden.reshape(-1, own, n_sp, rows, share)
    hidden = jnp.transpose(hidden, (0, 2, 1, 3, 4)).reshape(-1, share)
    partial_down = jnp.dot(hidden, down_full, preferred_element_type=jnp.float32)
    partial_down = partial_down.astype(jnp.bfloat16).reshape(-1, n_sp, own * rows, features)
    return reduce_rows(partial_down, mid, jnp.bfloat16, True).reshape(resid_in.shape)


def solution(mesh):
    placed = (
        P(("grp", "tp"), "sp", None),
        P("grp", "sp", "tp"),
        P("grp", "sp", "tp"),
        P("grp", "sp", "tp"),
        P("grp", "sp", "tp"),
        P("grp", "sp", "tp"),
        P("tp"),
        P(),
        P("grp", "sp"),
        P("tp", None),
        P(),
        P("sp", "tp"),
        P("sp", "tp"),
        P(None, "tp"),
        P(None, "tp"),
        P("tp", "sp"),
    )
    return jax.shard_map(
        per_device,
        mesh=mesh,
        in_specs=placed,
        out_specs=P(("grp", "tp"), "sp", None),
        check_vma=False,
    )
```
